32 devices in a mesh: grp: 2 (over y), ep: 4 (over z), tp: 4 (over x, core).
Axes of the slice: x: 2, y: 2, z: 4, core: 2. Of those that a mesh axis runs over, the one named last changes fastest.
Arguments:
- tokens: bfloat16 [2048, 2048], P(('grp', 'ep')), parts along dimension 0, may hold values from -6 to 6
- in_gain: bfloat16 [2048], replicated, may hold values from 0.099609375 to 1.8984375
- expert_ids: int32 [2048, 2], P(('grp', 'ep')), parts along dimension 0, may hold values from 0 to 3, all different within a row; in each aligned block of 256 rows (0 to 255, 256 to 511, ...) at most 256 rows name the same one
- route_weights: float32 [2048, 2], P(('grp', 'ep')), parts along dimension 0, may hold values from 0.1 to 1
- gate_weight: bfloat16 [4, 2048, 2048], P('ep', None, 'tp'), may hold values from -0.375 to 0.375
- up_weight: bfloat16 [4, 2048, 2048], P('ep', None, 'tp'), may hold values from -0.375 to 0.375
- down_weight: bfloat16 [4, 2048, 2048], P('ep', 'tp')
- out_gain: bfloat16 [2048], P('tp'), may hold values from 0.099609375 to 1.8984375
Outputs:
- normed_out: bfloat16 [2048, 2048], P(('grp', 'ep'), 'tp'), parts along dimension 0
The draws below stay inside these ranges and needn't reach their ends.
There are 2 independent parts, one for each index of `grp`. The reference program is written for one: setup_inputs(seed, part) draws one part's arguments, and reference() takes and returns one part's arrays. A program takes and returns all parts, laid end to end along the dimension named above; an argument that names none is the same for every part. Nothing has to cross between parts.
Inputs may be any that keep to these rules, and one draw needn't show every extreme that they name: `expert_ids`: each row names 2 different experts. Among the 256 rows of one index of ep, no expert is named more than 256 times, a bound that some block reaches.
All inputs are finite; a program needn't handle non-finite values.
Results may differ from the reference program's by a relative error of at most 0.015.
Values may be sent and summed in bfloat16 or wider, within the bound.
No kernel may reach another device: no remote copies, remote signals or barrier semaphores. Data moves between devices by JAX's collectives and lax.ppermute only.
A program may use at most 64 MiB of HBM per device.

```python
import math
import jax
import jax.numpy as jnp
import numpy as np
from jax import lax

D = 2048
FF = 2048
TOP_K = 2
TOK_DEV = 256
EXPERTS = 4
TOKENS = 1024
CAP = 256
N_EP = 4
N_TP = 4


def draw_down_weight(key, part):
    column = jnp.arange(D, dtype=jnp.float32) / D
    entries = jax.random.normal(key, (EXPERTS, FF, D), jnp.float32)
    scales = jnp.exp(jnp.log(4.0) * column)
    return (entries * scales[None, None, :] * FF ** (-0.5)).astype(jnp.bfloat16)


def level_of(stream_key, dims, shards, least, high):
    def one(position, shards_of):
        heights = jax.random.uniform(jax.random.fold_in(jax.random.fold_in(stream_key, 6), position), (shards_of,), jnp.float32, least / len(shards), high / len(shards))
        return jnp.repeat(jnp.exp(heights), dims[position] // shards_of).reshape((-1,) + (1,) * (len(dims) - position - 1))

    loudness = one(*shards[0])
    for cut in shards[1:]:
        loudness = loudness * one(*cut)
    return loudness


def routed_block(rng, own, number, rows, number_of, top, bound, slope):
    sequence = jax.random.permutation(rng, number_of)
    heavy_load, common = shares(number_of, rows * top, bound, slope, True), shares(number_of, rows * top, bound, slope, False)
    places = jnp.arange(number_of)

    def named(lengths, offset_by):
        used = int((lengths > 0).sum())
        fixed = max(1, used // 4)
        moved = fixed + (places - fixed + offset_by * (used - fixed)) % max(1, number_of - fixed)
        return jnp.zeros((number_of,), jnp.int32).at[sequence[jnp.where(places < fixed, places, moved)]].set(jnp.asarray(lengths, jnp.int32))

    lengths = jnp.where(number % 4 == 0, named(heavy_load, number // 4), named(common, number - number // 4 - 1))
    mixed = jax.random.permutation(jax.random.fold_in(own, 3), number_of)
    giver, taker = mixed[0:number_of // 2 * 2:2], mixed[1:number_of // 2 * 2:2]
    margin = jnp.minimum(lengths[giver] - 1, bound - lengths[taker]) // 2
    margin = jnp.where((giver == sequence[0]) | (taker == sequence[0]) | (lengths[taker] == 0), 0, jnp.maximum(margin, 0))
    moved = jax.random.randint(jax.random.fold_in(own, 4), (number_of // 2,), 0, 1 << 20) % (margin + 1)
    lengths = lengths.at[giver].add(-moved).at[taker].add(moved)
    items = jnp.searchsorted(jnp.cumsum(lengths), jnp.arange(rows * top), side="right").astype(jnp.int32)
    listing = items.reshape(top, rows).T
    listing = listing[jax.random.permutation(jax.random.fold_in(own, 1), rows)]
    offset_by = jax.random.randint(jax.random.fold_in(own, 2), (rows, 1), 0, top)
    return jnp.take_along_axis(listing, (jnp.arange(top)[None, :] + offset_by) % top, axis=1)


def shares(number_of, total, limit, lean, full):
    weights = [(1 << 20) // math.isqrt(grade ** lean) + 1 for grade in range(1, number_of + 1)]
    largest = limit if full else min(limit, max(-(-total // number_of), total * weights[0] // sum(weights)))
    least = 1 if total - largest >= number_of - 1 else 0
    given, surplus = [largest] + [least] * (number_of - 1), total - largest - least * (number_of - 1)
    while surplus > 0:
        free = [i for i in range(1, number_of) if given[i] < largest] or [i for i in range(1, number_of) if given[i] < limit]
        mass, left = sum([weights[i] for i in free]), surplus
        for i in free:
            addition = min(limit - given[i], max(1, left * weights[i] // mass), surplus)
            given[i] = given[i] + addition
            surplus = surplus - addition
    return np.array(given)


def centred(key, extent, spread, limit, cuts=(), kind=jnp.bfloat16):
    loudness = level_of(key, extent, cuts, -0.22, 0.18) if cuts else 1.0
    array = jax.random.normal(key, extent, jnp.float32) * spread * loudness
    return jnp.minimum(jnp.maximum(array, -limit), limit).astype(kind)


def setup_inputs(seed: int = 0, part: int = 0) -> dict:
    keys = jax.random.split(jax.random.key(seed), 9)
    part_splits = jax.random.split(jax.random.fold_in(keys[8], part), 9)
    tokens = centred(part_splits[0], (TOKENS, D), 1.0, 6.0, ((0, 4),))
    in_gain = jnp.clip(1.0 + 0.18 * jax.random.normal(keys[1], (D,), jnp.float32), 0.099609375, 1.8984375).astype(jnp.bfloat16)
    expert_ids_keys = jax.random.split(jax.random.fold_in(part_splits[2], 1), TOKENS // TOK_DEV)
    expert_ids_turns = jax.random.permutation(jax.random.fold_in(part_splits[2], 3), TOKENS // TOK_DEV)
    expert_ids = jax.vmap(lambda own, number: routed_block(jax.random.fold_in(part_splits[2], 2), own, number, TOK_DEV, EXPERTS, TOP_K, CAP, 2))(expert_ids_keys, expert_ids_turns).reshape((TOKENS, TOP_K))
    route_weights = jnp.clip(jnp.exp(math.log(1.0) - 2.3025851 * jax.random.uniform(part_splits[3], (TOKENS, TOP_K), jnp.float32) ** level_of(part_splits[3], (TOKENS, TOP_K), ((0, 4),), -0.2, 0.2)), 0.1, 1.0)
    gate_weight = centred(keys[4], (EXPERTS, D, FF), (D // 8) ** -0.5, 0.375, ((0, 4), (2, 4)))
    up_weight = centred(keys[5], (EXPERTS, D, FF), (D // 8) ** -0.5, 0.375, ((0, 4), (2, 4)))
    down_weight = draw_down_weight(jax.random.fold_in(keys[8], 71), part)
    out_gain = jnp.clip(1.0 + 0.18 * jax.random.normal(keys[7], (D,), jnp.float32), 0.099609375, 1.8984375).astype(jnp.bfloat16)
    return dict(tokens=tokens, in_gain=in_gain, expert_ids=expert_ids, route_weights=route_weights, gate_weight=gate_weight, up_weight=up_weight, down_weight=down_weight, out_gain=out_gain)


eps = 1e-05

def reference(tokens, in_gain, expert_ids, route_weights, gate_weight, up_weight, down_weight, out_gain):
    xf = tokens.astype(jnp.float32)
    normed_in = (xf * lax.rsqrt(lax.optimization_barrier(jnp.mean(xf * xf, axis=1, keepdims=True)) + eps) * in_gain.astype(jnp.float32)).astype(jnp.bfloat16)
    ids = expert_ids.reshape(N_EP, TOK_DEV * TOP_K)
    onehot = (ids[:, :, None] == jnp.arange(EXPERTS, dtype=jnp.int32)[None, None, :]).astype(jnp.int32)
    earlier = jnp.cumsum(onehot, axis=1) - onehot
    slot = lax.optimization_barrier(jnp.sum(earlier * onehot, axis=2))
    block = jnp.arange(N_EP, dtype=jnp.int32)[:, None]
    row_of = ((ids * N_EP + block) * CAP + slot).reshape(-1).astype(jnp.int32)
    token_of = (jnp.arange(TOKENS * TOP_K, dtype=jnp.int32) // TOP_K).astype(jnp.int32)
    row_token = jnp.full((EXPERTS * N_EP * CAP,), TOKENS, jnp.int32).at[row_of].set(token_of)
    row_token = row_token.reshape(EXPERTS, N_EP * CAP)
    extended = jnp.concatenate([normed_in, jnp.zeros((1, D), jnp.bfloat16)], axis=0)

    def expert_rows(args):
        picks, w_gate, w_up, w_down = args
        rows = extended[picks]
        gate_pre = jnp.dot(rows, w_gate, preferred_element_type=jnp.float32)
        up_pre = jnp.dot(rows, w_up, preferred_element_type=jnp.float32)
        g = jnp.minimum(gate_pre, 7.0)
        u = jnp.clip(up_pre, -7.0, 7.0)
        act = (g * jax.nn.sigmoid(1.702 * g) * (u + 1.0)).astype(jnp.bfloat16)
        groups = act.reshape(N_EP * CAP, N_TP, FF // N_TP).astype(jnp.float32)
        wd = w_down.reshape(N_TP, FF // N_TP, D).astype(jnp.float32)
        partial_value = jnp.einsum('rgf,gfd->grd', groups, wd).astype(jnp.bfloat16)
        return lax.optimization_barrier(jnp.sum(partial_value.astype(jnp.float32), axis=0)).astype(jnp.bfloat16)
    expert_out = lax.map(expert_rows, (row_token, gate_weight, up_weight, down_weight))
    expert_out = expert_out.reshape(EXPERTS * N_EP * CAP, D)
    picked = expert_out[row_of].astype(jnp.float32).reshape(TOKENS, TOP_K, D)
    combined = lax.optimization_barrier(jnp.sum(picked * route_weights[:, :, None], axis=1))
    scale = lax.rsqrt(lax.optimization_barrier(jnp.mean(combined * combined, axis=1, keepdims=True)) + eps)
    return (combined * scale * out_gain.astype(jnp.float32)).astype(jnp.bfloat16)
```

```python
import jax
import jax.numpy as jnp
from jax import lax
from jax.sharding import PartitionSpec as P

eps = 1e-05


def on_device_routed(
    tokens, in_gain, expert_ids, route_weights, gate_weight, up_weight, down_weight, out_gain
):
    n_ep = lax.axis_size("ep")
    n_tp = lax.axis_size("tp")
    tok_count, width = tokens.shape
    top_count = expert_ids.shape[1]
    experts = n_ep * gate_weight.shape[0]
    capacity = 2 * tok_count * top_count // experts
    feat_block = width // n_tp
    xf = tokens.astype(jnp.float32)
    normed_in = (
        xf * lax.rsqrt(jnp.mean(xf * xf, axis=1, keepdims=True) + eps) * in_gain.astype(jnp.float32)
    ).astype(jnp.bfloat16)
    flat_ids = expert_ids.reshape(-1)
    onehot = (flat_ids[:, None] == jnp.arange(experts, dtype=jnp.int32)[None, :]).astype(jnp.int32)
    slot = jnp.sum((jnp.cumsum(onehot, axis=0) - onehot) * onehot, axis=1)
    dest = flat_ids * capacity + slot
    token_of = jnp.arange(tok_count * top_count, dtype=jnp.int32) // top_count
    slot_token = jnp.full((experts * capacity,), tok_count, jnp.int32).at[dest].set(token_of)
    source = lax.dynamic_slice_in_dim(normed_in, lax.axis_index("tp") * feat_block, feat_block, 1)
    extended = jnp.concatenate([source, jnp.zeros((1, source.shape[1]), jnp.bfloat16)], axis=0)
    outgoing = extended[slot_token].reshape(experts, capacity, source.shape[1])
    w_gate = gate_weight[0]
    w_up = up_weight[0]
    arrived = lax.all_to_all(outgoing, "ep", split_axis=0, concat_axis=0, tiled=True).reshape(
        n_ep * capacity, feat_block
    )
    piece = lax.all_gather(arrived, "tp", axis=1, tiled=True)
    gate_pre = jnp.dot(piece, w_gate, preferred_element_type=jnp.float32)
    up_pre = jnp.dot(piece, w_up, preferred_element_type=jnp.float32)
    clamped = jnp.minimum(gate_pre, 7.0)
    bounded = jnp.clip(up_pre, -7.0, 7.0)
    act = (clamped * jax.nn.sigmoid(1.702 * clamped) * (bounded + 1.0)).astype(jnp.bfloat16)
    w_down = down_weight[0]
    summed = lax.psum_scatter(
        lax.dot_general(
            w_down, act, (((0,), (1,)), ((), ())), preferred_element_type=jnp.float32
        ).astype(jnp.bfloat16),
        "tp",
        scatter_dimension=0,
        tiled=True,
    )
    summed = summed.reshape(feat_block, n_ep, capacity)
    returned = lax.all_to_all(summed, "ep", split_axis=1, concat_axis=1, tiled=True)
    returned = returned.reshape(feat_block, experts * capacity).T
    picked = returned[dest].astype(jnp.float32).reshape(tok_count, top_count, feat_block)
    combined = jnp.sum(picked * route_weights[:, :, None], axis=1)
    squares = lax.psum(jnp.sum(combined * combined, axis=1), "tp")
    scale = lax.rsqrt(squares / width + eps)
    return (combined * scale[:, None] * out_gain.astype(jnp.float32)).astype(jnp.bfloat16)


def swap(value, axis, stride):
    count = lax.axis_size(axis)
    return lax.ppermute(value, axis, [(i, i ^ stride) for i in range(count)])


def shift(value, axis, by):
    count = lax.axis_size(axis)
    return lax.ppermute(value, axis, [(i, (i + by) % count) for i in range(count)])


def blocks_of(array, order, size, axis):
    return jnp.concatenate(
        [lax.dynamic_slice_in_dim(array, j * size, size, axis) for j in order], axis=axis
    )


def on_device_dense(
    tokens, in_gain, expert_ids, route_weights, gate_weight, up_weight, down_weight, out_gain
):
    n_ep = lax.axis_size("ep")
    n_tp = lax.axis_size("tp")
    me = lax.axis_index("tp")
    here = lax.axis_index("ep")
    tok_count, width = tokens.shape
    block = width // n_tp
    strides = []
    s = n_tp // 2
    while s:
        strides.append(s)
        s //= 2
    rel = [0]
    for s in strides:
        rel = rel + [r ^ s for r in rel]
    order = [me ^ r for r in rel]
    quarter = lax.dynamic_slice_in_dim(tokens, me * block, block, 1)
    hops = sorted(range(1, n_ep), key=lambda h: (min(h, n_ep - h), h))
    arrived = {h: shift(quarter, "ep", h) for h in hops}
    w_gate = blocks_of(gate_weight[0], order, block, 0)
    w_up = blocks_of(up_weight[0], order, block, 0)
    w_down = blocks_of(down_weight[0], order, block, 1)
    gain = blocks_of(in_gain, order, block, 0).astype(jnp.float32)

    def expert(x):
        xf = x.astype(jnp.float32)
        normed = (
            xf * lax.rsqrt(jnp.mean(xf * xf, axis=1, keepdims=True) + eps) * gain
        ).astype(jnp.bfloat16)
        gate_pre = jnp.dot(normed, w_gate, preferred_element_type=jnp.float32)
        up_pre = jnp.dot(normed, w_up, preferred_element_type=jnp.float32)
        g = jnp.minimum(gate_pre, 7.0)
        u = jnp.clip(up_pre, -7.0, 7.0)
        act = (g * jax.nn.sigmoid(1.702 * g) * (u + 1.0)).astype(jnp.bfloat16)
        part = jnp.dot(act, w_down, preferred_element_type=jnp.float32).astype(jnp.bfloat16)
        for s in reversed(strides):
            half = part.shape[1] // 2
            part = part[:, :half] + swap(part[:, half:], "tp", s)
        return part

    results = {0: expert(blocks_of(tokens, order, block, 1))}
    for h in hops:
        x = arrived[h]
        for s in strides:
            x = jnp.concatenate([x, swap(x, "tp", s)], axis=1)
        results[h] = shift(expert(x), "ep", -h)
    combined = jnp.zeros((tok_count, block), jnp.float32)
    for h in [0] + hops:
        named = expert_ids == (here + h) % n_ep
        weight = jnp.sum(jnp.where(named, route_weights, 0.0), axis=1, keepdims=True)
        taken = jnp.any(named, axis=1, keepdims=True)
        combined = combined + jnp.where(taken, weight * results[h].astype(jnp.float32), 0.0)
    squares = lax.psum(jnp.sum(combined * combined, axis=1), "tp")
    scale = lax.rsqrt(squares / width + eps)
    return (combined * scale[:, None] * out_gain.astype(jnp.float32)).astype(jnp.bfloat16)


def on_device(tokens, in_gain, expert_ids, route_weights, gate_weight, *rest):
    n_ep = lax.axis_size("ep")
    n_tp = lax.axis_size("tp")
    experts = n_ep * gate_weight.shape[0]
    capacity = 2 * tokens.shape[0] * expert_ids.shape[1] // experts
    dense = capacity >= tokens.shape[0] and gate_weight.shape[0] == 1 and n_tp & (n_tp - 1) == 0
    body = on_device_dense if dense else on_device_routed
    return body(tokens, in_gain, expert_ids, route_weights, gate_weight, *rest)


def solution(mesh):
    placed = (
        P(("grp", "ep"), None),
        P(),
        P(("grp", "ep"), None),
        P(("grp", "ep"), None),
        P("ep", None, "tp"),
        P("ep", None, "tp"),
        P("ep", "tp", None),
        P("tp"),
    )
    return jax.shard_map(
        on_device, mesh=mesh, in_specs=placed, out_specs=P(("grp", "ep"), "tp"), check_vma=False
    )
```
